256 devices in a mesh: sp: 32 (over z, x), dp: 8 (over y, core).
Axes of the slice: x: 4, y: 4, z: 8, core: 2. Of those that a mesh axis runs over, the one named last changes fastest.
Arguments:
- gate_in: bfloat16 [8, 16384, 4096], P('dp', 'sp'), may hold values from -6 to 6
- value_in: bfloat16 [8, 16384, 4096], P('dp', 'sp'), may hold values from -6 to 6
- segments: int32 [8, 16384], P('dp', 'sp'), may hold values from 0 to 7, never falling along the last dimension, each value on 1 to 3072 neighbouring positions
- value_gain: bfloat16 [4096], P('sp'), may hold values from 0.099609375 to 1.8984375
- mixing: bfloat16 [32, 1024, 1024], P('sp', 'dp'), may hold values from -0.1875 to 0.1875
- mixing_bias: bfloat16 [32, 1024], P('sp'), may hold values from 0.099609375 to 1.8984375
Outputs:
- gated: bfloat16 [8, 16384, 4096], P('dp', 'sp')
The draws below stay inside these ranges and needn't reach their ends.
Inputs may be any that keep to these rules, and one draw needn't show every extreme that they name: `segments`: within each sequence the numbers never fall, every number 0 to 7 occurs, a document spans at most 3072 positions and some document spans exactly that.
All inputs are finite; a program needn't handle non-finite values.
Results may differ from the reference program's by a relative error of at most 0.0054.
Values may be sent and summed in bfloat16 or wider, within the bound.
A program may use at most 128 MiB of HBM per device.

```python
import math
import jax
import jax.numpy as jnp
import numpy as np
from jax import lax

HEAD_DIM = 128
HEADS = 32
WIDTH = 4096
BLK = 1024
TOK_DEV = 512
SEQ = 16384
SEQS = 8
DOCS = 8


def steps_of(rng, dims, pieces, low, top_value):
    loudness, own = 1.0, jax.random.fold_in(rng, 6)
    for position, parts in pieces:
        heights = jnp.exp(jax.random.uniform(jax.random.fold_in(own, position), (parts,), jnp.float32, low / len(pieces), top_value / len(pieces)))
        loudness = loudness * jnp.repeat(heights, dims[position] // parts).reshape([-1 if axis == position else 1 for axis in range(len(dims))])
    return loudness


def split_up(count, total, reach, skew):
    portions = [(1 << 20) // math.isqrt(standing ** skew) + 1 for standing in range(2, count + 1)]
    spare, given = total - reach - (count - 1), [1] * (count - 1)
    while spare > 0:
        candidates = [i for i in range(count - 1) if given[i] < reach]
        whole, remaining = sum([portions[i] for i in candidates]), spare
        for i in candidates:
            extra = min(reach - given[i], max(1, remaining * portions[i] // whole), spare)
            given[i] = given[i] + extra
            spare = spare - extra
    return np.array([reach] + given)


def uneven(stream_key, number_of, total, bound, slope):
    if number_of == 2:
        one = jax.random.randint(stream_key, (), max(1, total - bound), min(bound, total - 1) + 1)
        return jnp.stack([one, total - one])
    sizes = jnp.asarray(split_up(number_of, total, bound, slope), jnp.int32)
    twos = (number_of - 1) // 2
    source_of, sink = sizes[1:1 + 2 * twos:2], sizes[2:2 + 2 * twos:2]
    margin = jnp.minimum(source_of - 1, bound - sink)
    shifted = jax.random.randint(jax.random.fold_in(stream_key, 1), (twos,), 0, 1 << 20) % (margin + 1)
    sizes = sizes.at[1:1 + 2 * twos:2].set(source_of - shifted).at[2:2 + 2 * twos:2].set(sink + shifted)
    return sizes[jax.random.permutation(jax.random.fold_in(stream_key, 2), number_of)]


def gaussian(key, shape, scale, limit, pieces=(), held_as=jnp.bfloat16):
    gain = steps_of(key, shape, pieces, -0.22, 0.18) if pieces else 1.0
    drawn = jax.random.normal(key, shape, jnp.float32) * scale * gain
    return jnp.minimum(jnp.maximum(drawn, -limit), limit).astype(held_as)


def setup_inputs(seed: int = 0) -> dict:
    seeds = jax.random.split(jax.random.key(seed), 7)
    gate_in = gaussian(seeds[0], (SEQS, SEQ, WIDTH), 1.0, 6.0, ((0, 8), (1, 32)))
    value_in = gaussian(seeds[1], (SEQS, SEQ, WIDTH), 1.0, 6.0, ((0, 8), (1, 32)))
    segments = jax.vmap(lambda own: jnp.searchsorted(jnp.cumsum(uneven(own, DOCS, SEQ, 6 * TOK_DEV, 0)), jnp.arange(SEQ), side="right"))(jax.random.split(seeds[2], SEQS)).reshape((SEQS, SEQ)).astype(jnp.int32)
    value_gain = jnp.clip(1.0 + 0.18 * jax.random.normal(seeds[3], (WIDTH,), jnp.float32), 0.099609375, 1.8984375).astype(jnp.bfloat16)
    mixing = gaussian(seeds[4], (HEADS, BLK, BLK), BLK ** -0.5, 0.1875, ((0, 32), (1, 8)))
    mixing_bias = jnp.clip(1.0 + 0.18 * jax.random.normal(seeds[5], (HEADS, BLK), jnp.float32), 0.099609375, 1.8984375).astype(jnp.bfloat16)
    return dict(gate_in=gate_in, value_in=value_in, segments=segments, value_gain=value_gain, mixing=mixing, mixing_bias=mixing_bias)


epsilon = 1e-06

def reference(gate_in, value_in, segments, value_gain, mixing, mixing_bias):
    seqs, length, width = value_in.shape
    values = jax.nn.gelu(value_in.astype(jnp.float32)).reshape(seqs, length, HEADS, HEAD_DIM)
    scaled = values * lax.rsqrt(lax.optimization_barrier(jnp.mean(values * values, axis=-1, keepdims=True)) + epsilon)
    normed = (scaled.reshape(seqs, length, width) * value_gain.astype(jnp.float32)).astype(jnp.bfloat16)
    blocks = seqs * length // BLK
    value_blocks = normed.reshape(blocks, BLK, HEADS, HEAD_DIM)
    id_blocks = segments.reshape(blocks, BLK)
    mixing_f = mixing.astype(jnp.float32)
    bias_f = jnp.transpose(mixing_bias.astype(jnp.float32))[:, :, None]

    def one_block(pair_item):
        block_values, block_ids = pair_item
        same_doc = block_ids[:, None] == block_ids[None, :]
        masked = jnp.where(same_doc[None, :, :], mixing_f, jnp.zeros((), jnp.float32))
        summed = jnp.einsum('hts,shd->thd', masked, block_values.astype(jnp.float32))
        return (summed + bias_f).astype(jnp.bfloat16)
    mixed = lax.map(one_block, (value_blocks, id_blocks)).reshape(seqs, length, width)
    gate_f = jax.nn.gelu(gate_in.astype(jnp.float32))
    return (gate_f * mixed.astype(jnp.float32)).astype(jnp.bfloat16)
```

```python
import jax
import jax.numpy as jnp
from jax import lax
from jax.experimental import pallas as pl
from jax.experimental.pallas import tpu as pltpu
from jax.sharding import PartitionSpec as P

MESH = pl.DeviceIdType.MESH
EPSILON = 1e-06
BF16, F32 = jnp.bfloat16, jnp.float32
NX, NY, NZ, NC = 4, 4, 8, 2
HD = 128
TOK = 512
BLK = 1024
HALF = 64
STEPS = 8


def gelu(x):
    inner = 0.7978845608028654 * (x + 0.044715 * (x * x * x))
    return x * (0.5 * (1.0 + jnp.tanh(inner)))


def kernel(
    gate_hbm,
    value_hbm,
    seg_hbm,
    aux_hbm,
    mix_hbm,
    out_ref,
    m_buf,
    v_buf,
    r_buf,
    o_buf,
    g_buf,
    mask_buf,
    vn_buf,
    col_buf,
    seg_buf,
    aux_buf,
    loc_sem,
    own_v_sem,
    seg_s,
    seg_r,
    v_s,
    v_r,
    r_s,
    r_r,
    a1_s,
    a1_r,
    a_s,
    a_r,
    b_s,
    b_r,
    x_s,
    x_r,
    b2_s,
    b2_r,
    c_s,
    c_r,
):
    sp, dp = lax.axis_index("sp"), lax.axis_index("dp")
    z, x = sp // NX, lax.rem(sp, NX)
    y, c = dp // NC, lax.rem(dp, NC)

    def x_peer(j):
        return {"sp": z * NX + lax.rem(x + j, NX), "dp": dp}

    def y_peer(j):
        return {"sp": sp, "dp": lax.rem(y + j, NY) * NC + c}

    def z_peer(j):
        return {"sp": lax.rem(z + j, NZ) * NX + x, "dp": dp}

    sibling = {"sp": sp, "dp": y * NC + (1 - c)}

    def remote(src, dst, ss, rs, dev):
        return pltpu.make_async_remote_copy(
            src_ref=src, dst_ref=dst, send_sem=ss, recv_sem=rs, device_id=dev, device_id_type=MESH
        )

    def head_z(k):
        far = (k + 1) // 2
        return lax.rem(z + jnp.where(lax.rem(k, 2) == 1, far, NZ - far), NZ)

    def head_cols(k, xs):
        return pl.ds(pl.multiple_of((head_z(k) * NX + xs) * HD, HD), HD)

    def x_rows(xs):
        return pl.ds(pl.multiple_of(xs * TOK, TOK), TOK)

    def v_send(k, j):
        xs = lax.rem(x + j, NX)
        return remote(
            value_hbm.at[0, :, head_cols(k, xs)],
            v_buf.at[k, x_rows(x)],
            v_s.at[k, j - 1],
            v_r.at[k, j - 1],
            x_peer(j),
        )

    def v_recv(k, j):
        xs = lax.rem(x + NX - j, NX)
        return remote(
            v_buf.at[k, x_rows(xs)], v_buf.at[k, x_rows(xs)], v_s.at[k, j - 1], v_r.at[k, j - 1], x_peer(j)
        )

    def r_send(k, j):
        xs = lax.rem(x + j, NX)
        return remote(
            r_buf.at[k, x_rows(xs)], o_buf.at[x, k], r_s.at[k, j - 1], r_r.at[k, j - 1], x_peer(j)
        )

    def r_recv(k, j):
        xs = lax.rem(x + NX - j, NX)
        return remote(o_buf.at[xs, k], o_buf.at[xs, k], r_s.at[k, j - 1], r_r.at[k, j - 1], x_peer(j))

    def seg_send(j):
        return remote(seg_hbm, seg_buf.at[x], seg_s.at[j - 1], seg_r.at[j - 1], x_peer(j))

    def seg_recv(j):
        xs = lax.rem(x + NX - j, NX)
        return remote(seg_buf.at[xs], seg_buf.at[xs], seg_s.at[j - 1], seg_r.at[j - 1], x_peer(j))

    def a1_send(j):
        return remote(
            mix_hbm.at[0, pl.ds(0, HALF)], m_buf.at[z, y, c, 0], a1_s.at[j - 1], a1_r.at[j - 1], y_peer(j)
        )

    def a1_recv(j):
        ref = m_buf.at[z, lax.rem(y + NY - j, NY), c, 0]
        return remote(ref, ref, a1_s.at[j - 1], a1_r.at[j - 1], y_peer(j))

    def a_msg(zh, ss, rs, dz):
        ref = m_buf.at[zh, :, c, 0]
        return remote(ref, ref, a_s.at[ss], a_r.at[rs], z_peer(dz))

    def a_half(zh, lo, ss, rs, dz):
        ref = m_buf.at[zh, pl.ds(lo, 2), c, 0]
        return remote(ref, ref, a_s.at[ss], a_r.at[rs], z_peer(dz))

    def b_msg(zh, ss, rs, dz):
        ref = m_buf.at[zh, y, c, 1]
        return remote(ref, ref, b_s.at[ss], b_r.at[rs], z_peer(dz))

    def b_half(zh, lo, ss, rs, dz):
        ref = m_buf.at[zh, y, c, 1, pl.ds(lo, HALF // 2)]
        return remote(ref, ref, b_s.at[ss], b_r.at[rs], z_peer(dz))

    def x_msg(zh, ss, rs, dz):
        ref = aux_buf.at[zh]
        return remote(ref, ref, x_s.at[ss], x_r.at[rs], z_peer(dz))

    def b2_send(k, j):
        ref = m_buf.at[head_z(k), y, c, 1]
        return remote(ref, ref, b2_s.at[k, j - 1], b2_r.at[k, j - 1], y_peer(j))

    def b2_recv(k, j):
        ref = m_buf.at[head_z(k), lax.rem(y + NY - j, NY), c, 1]
        return remote(ref, ref, b2_s.at[k, j - 1], b2_r.at[k, j - 1], y_peer(j))

    def c_send(k):
        ref = m_buf.at[head_z(k), :, c]
        return remote(ref, ref, c_s.at[k], c_r.at[k], sibling)

    def c_recv(k):
        ref = m_buf.at[head_z(k), :, 1 - c]
        return remote(ref, ref, c_s.at[k], c_r.at[k], sibling)

    barrier = pltpu.get_barrier_semaphore()
    peers = [x_peer(j) for j in (1, 2, 3)] + [y_peer(j) for j in (1, 2, 3)]
    peers += [z_peer(1), z_peer(NZ - 1), sibling]
    for peer in peers:
        pl.semaphore_signal(barrier, inc=1, device_id=peer, device_id_type=MESH)

    own_a = pltpu.make_async_copy(mix_hbm.at[0, pl.ds(0, HALF)], m_buf.at[z, y, c, 0], loc_sem.at[0])
    own_b = pltpu.make_async_copy(mix_hbm.at[0, pl.ds(HALF, HALF)], m_buf.at[z, y, c, 1], loc_sem.at[1])
    own_x = pltpu.make_async_copy(aux_hbm, aux_buf.at[z], loc_sem.at[2])
    own_seg = pltpu.make_async_copy(seg_hbm, seg_buf.at[x], loc_sem.at[3])
    own_gate = pltpu.make_async_copy(gate_hbm.at[0], g_buf, loc_sem.at[4])

    def own_v(k):
        return pltpu.make_async_copy(
            value_hbm.at[0, :, head_cols(k, x)], v_buf.at[k, x_rows(x)], own_v_sem.at[k]
        )

    own_a.start()
    own_b.start()
    own_x.start()
    own_seg.start()
    pl.semaphore_wait(barrier, len(peers))

    for j in (1, 2, 3):
        seg_send(j).start()
    for j in (1, 2, 3):
        a1_send(j).start()

    def start_v(k, carry):
        own_v(k).start()
        for j in (1, 3, 2):
            v_send(k, j).start()
        return carry

    lax.fori_loop(0, 2, start_v, 0)
    own_b.wait()
    own_x.wait()
    b_msg(z, 0, 1, NZ - 1).start()
    b_msg(z, 8, 2, 1).start()
    x_msg(z, 0, 1, NZ - 1).start()
    x_msg(z, 7, 2, 1).start()
    for j in (1, 2, 3):
        b2_send(0, j).start()
    lax.fori_loop(2, STEPS, start_v, 0)
    own_gate.start()

    own_seg.wait()
    for j in (1, 2, 3):
        seg_recv(j).wait_recv()

    def as_column(row):
        return jnp.transpose(jnp.broadcast_to(row, (HD, row.shape[1])))

    for s in range(NX):
        col_buf[pl.ds(lax.rem(s, 2) * TOK, TOK), :] = as_column(seg_buf[s].astype(F32))
        if s % 2 == 1:
            rows_ids = [seg_buf[s - 1].astype(F32), seg_buf[s].astype(F32)]

            def mask_rows(i, carry):
                rows = pl.ds(pl.multiple_of(i * 64, 64), 64)
                ids = col_buf[rows, :]
                for half in range(2):
                    for t in range(TOK // HD):
                        there = rows_ids[half][:, t * HD : (t + 1) * HD]
                        mask_buf[s // 2, rows, half * TOK + t * HD : half * TOK + (t + 1) * HD] = jnp.where(
                            ids == there, 1.0, 0.0
                        ).astype(BF16)
                return carry

            lax.fori_loop(0, BLK // 64, mask_rows, 0)

    def serve(k):
        zh = head_z(k)
        odd = lax.rem(k, 2) == 1

        @pl.when(k == 0)
        def _():
            own_a.wait()
            for j in (1, 2, 3):
                a1_recv(j).wait_recv()
            a_msg(z, 0, 1, NZ - 1).start()
            a_msg(z, 8, 2, 1).start()

        @pl.when((k >= 1) & (k <= 6))
        def _():
            a_msg(zh, k, k, 1).wait_recv()
            x_msg(zh, k, k, 1).wait_recv()
            b_msg(zh, k, k, 1).wait_recv()

        @pl.when((k >= 1) & (k <= 4))
        def _():
            dz = jnp.where(odd, NZ - 1, 1)
            a_msg(zh, k, k + 2, dz).start()
            x_msg(zh, k, k + 2, dz).start()
            b_msg(zh, k, k + 2, dz).start()

        @pl.when(k == 5)
        def _():
            a_half(zh, 0, 5, 7, NZ - 1).start()
            b_half(zh, 0, 5, 7, NZ - 1).start()
            x_msg(zh, 5, 7, NZ - 1).start()

        @pl.when(k == 6)
        def _():
            a_half(zh, 2, 6, 8, 1).start()
            b_half(zh, HALF // 2, 6, 8, 1).start()

        @pl.when(k == 7)
        def _():
            a_half(zh, 0, 7, 7, 1).wait_recv()
            a_half(zh, 2, 7, 8, 1).wait_recv()
            x_msg(zh, 7, 7, 1).wait_recv()
            b_half(zh, 0, 7, 7, 1).wait_recv()
            b_half(zh, HALF // 2, 7, 8, 1).wait_recv()

        @pl.when(k >= 1)
        def _():
            for j in (1, 2, 3):
                b2_send(k, j).start()

    def across(k):
        for j in (1, 2, 3):
            b2_recv(k, j).wait_recv()
        c_send(k).start()

    def compute(k):
        zh = head_z(k)
        own_v(k).wait()
        for j in (1, 2, 3):
            v_recv(k, j).wait_recv()
        aux = aux_buf[zh]
        gain = aux[:, BLK:]
        for t in range(BLK // TOK):
            col_buf[pl.ds(t * TOK, TOK), :] = as_column(aux[:, t * TOK : (t + 1) * TOK])

        def norm_rows(i, carry):
            rows = pl.ds(pl.multiple_of(i * 128, 128), 128)
            act = gelu(v_buf[k, rows, :].astype(F32))
            scaled = act * lax.rsqrt(jnp.mean(act * act, axis=-1, keepdims=True) + EPSILON)
            vn_buf[rows, :] = (scaled * gain).astype(BF16)
            return carry

        lax.fori_loop(0, NX * TOK // 128, norm_rows, 0)
        c_recv(k).wait_recv()

        def mix_rows(i, carry):
            block, part = i // NY, lax.rem(i, NY)
            rows = pl.ds(pl.multiple_of(part * 256, 256), 256)
            matrix = m_buf[zh, part].reshape(256, BLK) * mask_buf[block, rows, :]
            values = vn_buf[pl.ds(pl.multiple_of(block * BLK, BLK), BLK), :]
            summed = jnp.dot(matrix, values, preferred_element_type=F32)
            r_buf[k, pl.ds(pl.multiple_of(block * BLK + part * 256, 256), 256), :] = (
                summed + col_buf[rows, :]
            ).astype(BF16)
            return carry

        lax.fori_loop(0, 2 * NY, mix_rows, 0)
        for j in (1, 3, 2):
            r_send(k, j).start()

    def step(i, carry):
        @pl.when(i < STEPS)
        def _():
            serve(i)

        @pl.when((i >= 1) & (i <= STEPS))
        def _():
            across(i - 1)

        @pl.when(i >= 2)
        def _():
            compute(i - 2)

        return carry

    lax.fori_loop(0, STEPS + 2, step, 0)

    own_gate.wait()

    def gate_rows(k, xs, source):
        cols = head_cols(k, xs)
        for i in range(TOK // 128):
            rows = pl.ds(i * 128, 128)
            gate = gelu(g_buf[rows, cols].astype(F32))
            out_ref[0, rows, cols] = (gate * source(i * 128).astype(F32)).astype(BF16)

    def own_gated(k, carry):
        gate_rows(
            k, x, lambda lo: r_buf[k, pl.ds(pl.multiple_of(x * TOK + lo, 128), 128), :]
        )
        return carry

    lax.fori_loop(0, STEPS, own_gated, 0)

    def gated(k, carry):
        for j in (1, 3, 2):
            r_recv(k, j).wait_recv()
            xs = lax.rem(x + NX - j, NX)
            gate_rows(k, xs, lambda lo: o_buf[xs, k, pl.ds(lo, 128), :])
        return carry

    lax.fori_loop(0, STEPS, gated, 0)

    def sent(k, carry):
        for j in (1, 2, 3):
            v_send(k, j).wait_send()
            r_send(k, j).wait_send()
            b2_send(k, j).wait_send()
        c_send(k).wait_send()
        return carry

    lax.fori_loop(0, STEPS, sent, 0)
    for j in (1, 2, 3):
        seg_send(j).wait_send()
        a1_send(j).wait_send()
    for k in (0, 1, 2, 3, 4, 8):
        a_msg(z, k, 0, 1).wait_send()
        b_msg(z, k, 0, 1).wait_send()
    for k in (5, 6):
        a_half(z, 0, k, 0, 1).wait_send()
        b_half(z, 0, k, 0, 1).wait_send()
    for k in (0, 1, 2, 3, 4, 5, 7):
        x_msg(z, k, 0, 1).wait_send()


def per_device(gate_in, value_in, segments, value_gain, mixing, mixing_bias):
    aux = jnp.concatenate([mixing_bias.astype(F32), value_gain.astype(F32)[None, :]], axis=1)
    any_space = pl.BlockSpec(memory_space=pl.ANY)
    dma = pltpu.SemaphoreType.DMA
    return pl.pallas_call(
        kernel,
        out_shape=jax.ShapeDtypeStruct(value_in.shape, BF16),
        in_specs=[any_space] * 5,
        out_specs=pl.BlockSpec(memory_space=pltpu.VMEM),
        scratch_shapes=[
            pltpu.VMEM((NZ, NY, NC, 2, HALF, BLK), BF16),
            pltpu.VMEM((STEPS, NX * TOK, HD), BF16),
            pltpu.VMEM((STEPS, NX * TOK, HD), BF16),
            pltpu.VMEM((NX, STEPS, TOK, HD), BF16),
            pltpu.VMEM((TOK, NX * NZ * HD), BF16),
            pltpu.VMEM((2, BLK, BLK), BF16),
            pltpu.VMEM((NX * TOK, HD), BF16),
            pltpu.VMEM((BLK, HD), F32),
            pltpu.VMEM((NX, 1, TOK), jnp.int32),
            pltpu.VMEM((NZ, 1, BLK + HD), F32),
            dma((5,)),
            dma((STEPS,)),
            dma((3,)),
            dma((3,)),
            dma((STEPS, 3)),
            dma((STEPS, 3)),
            dma((STEPS, 3)),
            dma((STEPS, 3)),
            dma((3,)),
            dma((3,)),
            dma((9,)),
            dma((9,)),
            dma((9,)),
            dma((9,)),
            dma((8,)),
            dma((8,)),
            dma((STEPS, 3)),
            dma((STEPS, 3)),
            dma((STEPS,)),
            dma((STEPS,)),
        ],
        compiler_params=pltpu.CompilerParams(
            collective_id=0, has_side_effects=True, vmem_limit_bytes=60 * 1024 * 1024
        ),
    )(gate_in, value_in, segments, aux, mixing)


def solution(mesh):
    return jax.shard_map(
        per_device,
        mesh=mesh,
        in_specs=(
            P("dp", "sp", None),
            P("dp", "sp", None),
            P("dp", "sp"),
            P("sp"),
            P("sp", "dp", None),
            P("sp", None),
        ),
        out_specs=P("dp", "sp", None),
        check_vma=False,
    )
```

```python
import jax
import jax.numpy as jnp
from jax import lax
from jax.experimental import pallas as pl
from jax.experimental.pallas import tpu as pltpu
from jax.sharding import PartitionSpec as P

MESH = pl.DeviceIdType.MESH
EPSILON = 1e-06
BF16, F32 = jnp.bfloat16, jnp.float32
NX, NY, NZ, NC = 4, 4, 8, 2
HD = 128
TOK = 512
BLK = 1024
HALF = 64
STEPS = 8


def gelu(x):
    inner = 0.7978845608028654 * (x + 0.044715 * (x * x * x))
    return x * (0.5 * (1.0 + jnp.tanh(inner)))


def kernel(
    gate_hbm,
    value_hbm,
    seg_hbm,
    gain_hbm,
    mix_hbm,
    bias_hbm,
    out_ref,
    m_buf,
    v_buf,
    r_buf,
    o_buf,
    g_buf,
    mask_buf,
    vn_buf,
    col_buf,
    seg_buf,
    bias_buf,
    gain_buf,
    loc_sem,
    own_v_sem,
    seg_s,
    seg_r,
    v_s,
    v_r,
    r_s,
    r_r,
    a1_s,
    a1_r,
    a_s,
    a_r,
    b_s,
    b_r,
    bias_s,
    bias_r,
    gain_s,
    gain_r,
    b2_s,
    b2_r,
    c_s,
    c_r,
    row_sem,
    far_sem,
):
    sp, dp = lax.axis_index("sp"), lax.axis_index("dp")
    z, x = sp // NX, lax.rem(sp, NX)
    y, c = dp // NC, lax.rem(dp, NC)

    def x_peer(j):
        return {"sp": z * NX + lax.rem(x + j, NX), "dp": dp}

    def y_peer(j):
        return {"sp": sp, "dp": lax.rem(y + j, NY) * NC + c}

    def z_peer(j):
        return {"sp": lax.rem(z + j, NZ) * NX + x, "dp": dp}

    sibling = {"sp": sp, "dp": y * NC + (1 - c)}

    def remote(src, dst, ss, rs, dev):
        return pltpu.make_async_remote_copy(
            src_ref=src, dst_ref=dst, send_sem=ss, recv_sem=rs, device_id=dev, device_id_type=MESH
        )

    def head_z(k):
        far = (k + 1) // 2
        return lax.rem(z + jnp.where(lax.rem(k, 2) == 1, far, NZ - far), NZ)

    def head_cols(k, xs):
        return pl.ds(pl.multiple_of((head_z(k) * NX + xs) * HD, HD), HD)

    def x_rows(xs):
        return pl.ds(pl.multiple_of(xs * TOK, TOK), TOK)

    def v_send(k, j):
        xs = lax.rem(x + j, NX)
        return remote(
            value_hbm.at[0, :, head_cols(k, xs)],
            v_buf.at[k, x_rows(x)],
            v_s.at[k, j - 1],
            v_r.at[k, j - 1],
            x_peer(j),
        )

    def v_recv(k, j):
        xs = lax.rem(x + NX - j, NX)
        return remote(
            v_buf.at[k, x_rows(xs)], v_buf.at[k, x_rows(xs)], v_s.at[k, j - 1], v_r.at[k, j - 1], x_peer(j)
        )

    def r_send(k, j):
        xs = lax.rem(x + j, NX)
        return remote(
            r_buf.at[k, x_rows(xs)], o_buf.at[x, k], r_s.at[k, j - 1], r_r.at[k, j - 1], x_peer(j)
        )

    def r_recv(k, j):
        xs = lax.rem(x + NX - j, NX)
        return remote(o_buf.at[xs, k], o_buf.at[xs, k], r_s.at[k, j - 1], r_r.at[k, j - 1], x_peer(j))

    def seg_send(j):
        return remote(seg_hbm, seg_buf.at[x], seg_s.at[j - 1], seg_r.at[j - 1], x_peer(j))

    def seg_recv(j):
        xs = lax.rem(x + NX - j, NX)
        return remote(seg_buf.at[xs], seg_buf.at[xs], seg_s.at[j - 1], seg_r.at[j - 1], x_peer(j))

    def a1_send(j):
        return remote(
            mix_hbm.at[0, pl.ds(0, HALF)], m_buf.at[z, y, c, 0], a1_s.at[j - 1], a1_r.at[j - 1], y_peer(j)
        )

    def a1_recv(j):
        ref = m_buf.at[z, lax.rem(y + NY - j, NY), c, 0]
        return remote(ref, ref, a1_s.at[j - 1], a1_r.at[j - 1], y_peer(j))

    def a_msg(zh, ss, rs, dz):
        ref = m_buf.at[zh, :, c, 0]
        return remote(ref, ref, a_s.at[ss], a_r.at[rs], z_peer(dz))

    def a_half(zh, lo, ss, rs, dz):
        ref = m_buf.at[zh, pl.ds(lo, 2), c, 0]
        return remote(ref, ref, a_s.at[ss], a_r.at[rs], z_peer(dz))

    def b_msg(zh, ss, rs, dz):
        ref = m_buf.at[zh, y, c, 1]
        return remote(ref, ref, b_s.at[ss], b_r.at[rs], z_peer(dz))

    def b_half(zh, lo, ss, rs, dz):
        ref = m_buf.at[zh, y, c, 1, pl.ds(lo, HALF // 2)]
        return remote(ref, ref, b_s.at[ss], b_r.at[rs], z_peer(dz))

    def x_msgs(zh, ss, rs, dz):
        bias, gain = bias_buf.at[zh], gain_buf.at[zh]
        return (
            remote(bias, bias, bias_s.at[ss], bias_r.at[rs], z_peer(dz)),
            remote(gain, gain, gain_s.at[ss], gain_r.at[rs], z_peer(dz)),
        )

    def b2_send(k, j):
        ref = m_buf.at[head_z(k), y, c, 1]
        return remote(ref, ref, b2_s.at[k, j - 1], b2_r.at[k, j - 1], y_peer(j))

    def b2_recv(k, j):
        ref = m_buf.at[head_z(k), lax.rem(y + NY - j, NY), c, 1]
        return remote(ref, ref, b2_s.at[k, j - 1], b2_r.at[k, j - 1], y_peer(j))

    def c_send(k):
        ref = m_buf.at[head_z(k), :, c]
        return remote(ref, ref, c_s.at[k], c_r.at[k], sibling)

    def c_recv(k):
        ref = m_buf.at[head_z(k), :, 1 - c]
        return remote(ref, ref, c_s.at[k], c_r.at[k], sibling)

    barrier = pltpu.get_barrier_semaphore()

    def tell(peer, core):
        there = {"sp": peer["sp"], "dp": peer["dp"] // NC * NC + core}
        pl.semaphore_signal(barrier, inc=1, device_id=there, device_id_type=MESH)

    @pl.when(c == 0)
    def _():
        pl.semaphore_signal(barrier, inc=1, device_id=sibling, device_id_type=MESH)

    for j in (1, 2, 3):
        tell(x_peer(j), 1)
    for peer in [z_peer(1), z_peer(NZ - 1)] + [y_peer(j) for j in (1, 2, 3)]:
        tell(peer, 0)

    own_a = pltpu.make_async_copy(mix_hbm.at[0, pl.ds(0, HALF)], m_buf.at[z, y, c, 0], loc_sem.at[0])
    own_b = pltpu.make_async_copy(mix_hbm.at[0, pl.ds(HALF, HALF)], m_buf.at[z, y, c, 1], loc_sem.at[1])
    own_bias = pltpu.make_async_copy(bias_hbm, bias_buf.at[z], loc_sem.at[2])
    own_seg = pltpu.make_async_copy(seg_hbm, seg_buf.at[x], loc_sem.at[3])
    own_gate = pltpu.make_async_copy(gate_hbm.at[0], g_buf, loc_sem.at[4])
    own_gain = pltpu.make_async_copy(gain_hbm, gain_buf.at[z], loc_sem.at[5])

    def own_v(k):
        return pltpu.make_async_copy(
            value_hbm.at[0, :, head_cols(k, x)], v_buf.at[k, x_rows(x)], own_v_sem.at[k]
        )

    for own in (own_b, own_a, own_bias, own_gain, own_seg):
        own.start()

    @pl.when(c == 1)
    def _():
        pl.semaphore_wait(barrier, 7)
        pl.semaphore_signal(row_sem, inc=1, device_id=sibling, device_id_type=MESH)

    @pl.when(c == 0)
    def _():
        pl.semaphore_wait(row_sem, 1)

    def start_v(k, carry):
        for j in (1, 3, 2):
            v_send(k, j).start()
        return carry

    def start_own_v(k, carry):
        own_v(k).start()
        return carry

    lax.fori_loop(0, 1, start_v, 0)
    for j in (1, 2, 3):
        seg_send(j).start()
    lax.fori_loop(1, STEPS, start_v, 0)

    @pl.when(c == 0)
    def _():
        pl.semaphore_wait(barrier, 10)
        pl.semaphore_signal(far_sem, inc=1, device_id=sibling, device_id_type=MESH)

    @pl.when(c == 1)
    def _():
        pl.semaphore_wait(far_sem, 1)

    for j in (1, 2, 3):
        a1_send(j).start()
    own_b.wait()
    b_msg(z, 0, 1, NZ - 1).start()
    b_msg(z, 8, 2, 1).start()
    own_bias.wait()
    own_gain.wait()
    for small in x_msgs(z, 0, 1, NZ - 1) + x_msgs(z, 7, 2, 1):
        small.start()
    for j in (1, 2, 3):
        b2_send(0, j).start()
    lax.fori_loop(0, STEPS, start_own_v, 0)
    own_gate.start()

    own_seg.wait()
    for j in (1, 2, 3):
        seg_recv(j).wait_recv()

    def as_column(row):
        return jnp.transpose(jnp.broadcast_to(row, (HD, row.shape[1])))

    for s in range(NX):
        col_buf[pl.ds(lax.rem(s, 2) * TOK, TOK), :] = as_column(seg_buf[s].astype(F32))
        if s % 2 == 1:
            rows_ids = [seg_buf[s - 1].astype(F32), seg_buf[s].astype(F32)]

            def mask_rows(i, carry):
                rows = pl.ds(pl.multiple_of(i * 64, 64), 64)
                ids = col_buf[rows, :]
                for half in range(2):
                    for t in range(TOK // HD):
                        there = rows_ids[half][:, t * HD : (t + 1) * HD]
                        mask_buf[s // 2, rows, half * TOK + t * HD : half * TOK + (t + 1) * HD] = jnp.where(
                            ids == there, 1.0, 0.0
                        ).astype(BF16)
                return carry

            lax.fori_loop(0, BLK // 64, mask_rows, 0)

    def serve(k):
        zh = head_z(k)
        odd = lax.rem(k, 2) == 1

        @pl.when(k == 0)
        def _():
            own_a.wait()
            for j in (1, 2, 3):
                a1_recv(j).wait_recv()
            a_msg(z, 0, 1, NZ - 1).start()
            a_msg(z, 8, 2, 1).start()

        @pl.when((k >= 1) & (k <= 6))
        def _():
            a_msg(zh, k, k, 1).wait_recv()
            for small in x_msgs(zh, k, k, 1):
                small.wait_recv()
            b_msg(zh, k, k, 1).wait_recv()

        @pl.when((k >= 1) & (k <= 4))
        def _():
            dz = jnp.where(odd, NZ - 1, 1)
            a_msg(zh, k, k + 2, dz).start()
            for small in x_msgs(zh, k, k + 2, dz):
                small.start()
            b_msg(zh, k, k + 2, dz).start()

        @pl.when(k == 5)
        def _():
            a_half(zh, 0, 5, 7, NZ - 1).start()
            b_half(zh, 0, 5, 7, NZ - 1).start()
            for small in x_msgs(zh, 5, 7, NZ - 1):
                small.start()

        @pl.when(k == 6)
        def _():
            a_half(zh, 2, 6, 8, 1).start()
            b_half(zh, HALF // 2, 6, 8, 1).start()

        @pl.when(k == 7)
        def _():
            a_half(zh, 0, 7, 7, 1).wait_recv()
            a_half(zh, 2, 7, 8, 1).wait_recv()
            for small in x_msgs(zh, 7, 7, 1):
                small.wait_recv()
            b_half(zh, 0, 7, 7, 1).wait_recv()
            b_half(zh, HALF // 2, 7, 8, 1).wait_recv()

        @pl.when(k >= 1)
        def _():
            for j in (1, 2, 3):
                b2_send(k, j).start()

    def across(k):
        for j in (1, 2, 3):
            b2_recv(k, j).wait_recv()
        c_send(k).start()

    def compute(k):
        zh = head_z(k)
        own_v(k).wait()
        for j in (1, 2, 3):
            v_recv(k, j).wait_recv()
        gain = gain_buf[zh].astype(F32)
        bias = bias_buf[zh].astype(F32)
        for t in range(BLK // TOK):
            col_buf[pl.ds(t * TOK, TOK), :] = as_column(bias[:, t * TOK : (t + 1) * TOK])

        def norm_rows(i, carry):
            rows = pl.ds(pl.multiple_of(i * 128, 128), 128)
            act = gelu(v_buf[k, rows, :].astype(F32))
            scaled = act * lax.rsqrt(jnp.mean(act * act, axis=-1, keepdims=True) + EPSILON)
            vn_buf[rows, :] = (scaled * gain).astype(BF16)
            return carry

        lax.fori_loop(0, NX * TOK // 128, norm_rows, 0)
        c_recv(k).wait_recv()

        def mix_rows(i, carry):
            block, part = i // NY, lax.rem(i, NY)
            rows = pl.ds(pl.multiple_of(part * 256, 256), 256)
            matrix = m_buf[zh, part].reshape(256, BLK) * mask_buf[block, rows, :]
            values = vn_buf[pl.ds(pl.multiple_of(block * BLK, BLK), BLK), :]
            summed = jnp.dot(matrix, values, preferred_element_type=F32)
            r_buf[k, pl.ds(pl.multiple_of(block * BLK + part * 256, 256), 256), :] = (
                summed + col_buf[rows, :]
            ).astype(BF16)
            return carry

        lax.fori_loop(0, 2 * NY, mix_rows, 0)
        for j in (1, 3, 2):
            r_send(k, j).start()

    def step(i, carry):
        @pl.when(i < STEPS)
        def _():
            serve(i)

        @pl.when((i >= 1) & (i <= STEPS))
        def _():
            across(i - 1)

        @pl.when(i >= 2)
        def _():
            compute(i - 2)

        return carry

    lax.fori_loop(0, STEPS + 2, step, 0)

    own_gate.wait()

    def gate_rows(k, xs, source):
        cols = head_cols(k, xs)
        for i in range(TOK // 128):
            rows = pl.ds(i * 128, 128)
            gate = gelu(g_buf[rows, cols].astype(F32))
            out_ref[0, rows, cols] = (gate * source(i * 128).astype(F32)).astype(BF16)

    def own_gated(k, carry):
        gate_rows(
            k, x, lambda lo: r_buf[k, pl.ds(pl.multiple_of(x * TOK + lo, 128), 128), :]
        )
        return carry

    lax.fori_loop(0, STEPS, own_gated, 0)

    def gated(k, carry):
        for j in (1, 3, 2):
            r_recv(k, j).wait_recv()
            xs = lax.rem(x + NX - j, NX)
            gate_rows(k, xs, lambda lo: o_buf[xs, k, pl.ds(lo, 128), :])
        return carry

    lax.fori_loop(0, STEPS, gated, 0)

    def sent(k, carry):
        for j in (1, 2, 3):
            v_send(k, j).wait_send()
            r_send(k, j).wait_send()
            b2_send(k, j).wait_send()
        c_send(k).wait_send()
        return carry

    lax.fori_loop(0, STEPS, sent, 0)
    for j in (1, 2, 3):
        seg_send(j).wait_send()
        a1_send(j).wait_send()
    for k in (0, 1, 2, 3, 4, 8):
        a_msg(z, k, 0, 1).wait_send()
        b_msg(z, k, 0, 1).wait_send()
    for k in (5, 6):
        a_half(z, 0, k, 0, 1).wait_send()
        b_half(z, 0, k, 0, 1).wait_send()
    for k in (0, 1, 2, 3, 4, 5, 7):
        for small in x_msgs(z, k, 0, 1):
            small.wait_send()


def per_device(gate_in, value_in, segments, value_gain, mixing, mixing_bias):
    any_space = pl.BlockSpec(memory_space=pl.ANY)
    dma = pltpu.SemaphoreType.DMA
    return pl.pallas_call(
        kernel,
        out_shape=pltpu.VMEM(value_in.shape, BF16),
        in_specs=[any_space] * 6,
        out_specs=pl.BlockSpec(memory_space=pltpu.VMEM),
        scratch_shapes=[
            pltpu.VMEM((NZ, NY, NC, 2, HALF, BLK), BF16),
            pltpu.VMEM((STEPS, NX * TOK, HD), BF16),
            pltpu.VMEM((STEPS, NX * TOK, HD), BF16),
            pltpu.VMEM((NX, STEPS, TOK, HD), BF16),
            pltpu.VMEM((TOK, NX * NZ * HD), BF16),
            pltpu.VMEM((2, BLK, BLK), BF16),
            pltpu.VMEM((NX * TOK, HD), BF16),
            pltpu.VMEM((BLK, HD), F32),
            pltpu.VMEM((NX, 1, TOK), jnp.int32),
            pltpu.VMEM((NZ, 1, BLK), BF16),
            pltpu.VMEM((NZ, 1, HD), BF16),
            dma((6,)),
            dma((STEPS,)),
            dma((3,)),
            dma((3,)),
            dma((STEPS, 3)),
            dma((STEPS, 3)),
            dma((STEPS, 3)),
            dma((STEPS, 3)),
            dma((3,)),
            dma((3,)),
            dma((9,)),
            dma((9,)),
            dma((9,)),
            dma((9,)),
            dma((8,)),
            dma((8,)),
            dma((8,)),
            dma((8,)),
            dma((STEPS, 3)),
            dma((STEPS, 3)),
            dma((STEPS,)),
            dma((STEPS,)),
            pltpu.SemaphoreType.REGULAR,
            pltpu.SemaphoreType.REGULAR,
        ],
        compiler_params=pltpu.CompilerParams(
            collective_id=0, has_side_effects=True, vmem_limit_bytes=48 * 1024 * 1024
        ),
    )(*(pltpu.with_memory_space_constraint(a, pltpu.HBM) for a in (gate_in, value_in, segments, value_gain.reshape(1, HD), mixing, mixing_bias)))


def solution(mesh):
    return jax.shard_map(
        per_device,
        mesh=mesh,
        in_specs=(
            P("dp", "sp", None),
            P("dp", "sp", None),
            P("dp", "sp"),
            P("sp"),
            P("sp", "dp", None),
            P("sp", None),
        ),
        out_specs=P("dp", "sp", None),
        check_vma=False,
    )
```

```python
import jax
import jax.numpy as jnp
from jax import lax
from jax.experimental import pallas as pl
from jax.experimental.pallas import tpu as pltpu
from jax.sharding import PartitionSpec as P

MESH = pl.DeviceIdType.MESH
EPSILON = 1e-06
BF16, F32 = jnp.bfloat16, jnp.float32
NX, NY, NZ, NC = 4, 4, 8, 2
HD = 128
TOK = 512
BLK = 1024
HALF = 64
STEPS = 8
INBOX_X = 0


def gelu(x):
    inner = 0.7978845608028654 * (x + 0.044715 * (x * x * x))
    return x * (0.5 * (1.0 + jnp.tanh(inner)))


def kernel(
    gate_hbm,
    value_hbm,
    seg_hbm,
    gain_hbm,
    mix_hbm,
    bias_hbm,
    out_ref,
    m_buf,
    v_buf,
    r_buf,
    o_buf,
    g_buf,
    mask_buf,
    vn_buf,
    col_buf,
    seg_buf,
    bias_buf,
    gain_buf,
    loc_sem,
    own_v_sem,
    seg_s,
    seg_r,
    v_s,
    v_r,
    r_s,
    r_r,
    a1_s,
    a1_r,
    a_s,
    a_r,
    b_s,
    b_r,
    bias_s,
    bias_r,
    gain_s,
    gain_r,
    b2_s,
    b2_r,
    c_s,
    c_r,
    row_sem,
    far_sem,
):
    sp, dp = lax.axis_index("sp"), lax.axis_index("dp")
    z, x = sp // NX, lax.rem(sp, NX)
    y, c = dp // NC, lax.rem(dp, NC)

    def x_peer(j):
        return {"sp": z * NX + lax.rem(x + j, NX), "dp": dp}

    def y_peer(j):
        return {"sp": sp, "dp": lax.rem(y + j, NY) * NC + c}

    def z_peer(j):
        return {"sp": lax.rem(z + j, NZ) * NX + x, "dp": dp}

    sibling = {"sp": sp, "dp": y * NC + (1 - c)}

    def remote(src, dst, ss, rs, dev):
        return pltpu.make_async_remote_copy(
            src_ref=src, dst_ref=dst, send_sem=ss, recv_sem=rs, device_id=dev, device_id_type=MESH
        )

    def head_z(k):
        far = (k + 1) // 2
        return lax.rem(z + jnp.where(lax.rem(k, 2) == 1, far, NZ - far), NZ)

    def head_cols(k, xs):
        return pl.ds(pl.multiple_of((head_z(k) * NX + xs) * HD, HD), HD)

    def x_rows(xs):
        return pl.ds(pl.multiple_of(xs * TOK, TOK), TOK)

    def v_send(k, j):
        xs = lax.rem(x + j, NX)
        return remote(
            value_hbm.at[0, :, head_cols(k, xs)],
            v_buf.at[k, x_rows(x)],
            v_s.at[k, j - 1],
            v_r.at[k, j - 1],
            x_peer(j),
        )

    def v_recv(k, j):
        xs = lax.rem(x + NX - j, NX)
        return remote(
            v_buf.at[k, x_rows(xs)], v_buf.at[k, x_rows(xs)], v_s.at[k, j - 1], v_r.at[k, j - 1], x_peer(j)
        )

    def r_send(k, j):
        xs = lax.rem(x + j, NX)
        return remote(
            r_buf.at[k, x_rows(xs)], o_buf.at[x, k], r_s.at[k, j - 1], r_r.at[k, j - 1], x_peer(j)
        )

    def r_recv(k, j):
        xs = lax.rem(x + NX - j, NX)
        return remote(o_buf.at[xs, k], o_buf.at[xs, k], r_s.at[k, j - 1], r_r.at[k, j - 1], x_peer(j))

    def seg_send(j):
        return remote(seg_hbm, seg_buf.at[x], seg_s.at[j - 1], seg_r.at[j - 1], x_peer(j))

    def seg_recv(j):
        xs = lax.rem(x + NX - j, NX)
        return remote(seg_buf.at[xs], seg_buf.at[xs], seg_s.at[j - 1], seg_r.at[j - 1], x_peer(j))

    def a1_send(j):
        return remote(
            mix_hbm.at[0, pl.ds(0, HALF)], m_buf.at[z, y, c, 0], a1_s.at[j - 1], a1_r.at[j - 1], y_peer(j)
        )

    def a1_recv(j):
        ref = m_buf.at[z, lax.rem(y + NY - j, NY), c, 0]
        return remote(ref, ref, a1_s.at[j - 1], a1_r.at[j - 1], y_peer(j))

    def a_msg(zh, half, ss, rs, dz):
        ref = m_buf.at[zh, pl.ds(2 * half, 2), c, 0]
        return remote(ref, ref, a_s.at[ss], a_r.at[rs], z_peer(dz))

    def b_msg(zh, ss, rs, dz):
        ref = m_buf.at[zh, y, c, 1]
        return remote(ref, ref, b_s.at[ss], b_r.at[rs], z_peer(dz))

    def b_half(zh, lo, ss, rs, dz):
        ref = m_buf.at[zh, y, c, 1, pl.ds(lo, HALF // 2)]
        return remote(ref, ref, b_s.at[ss], b_r.at[rs], z_peer(dz))

    def x_msgs(zh, ss, rs, dz):
        bias, gain = bias_buf.at[zh], gain_buf.at[zh]
        return (
            remote(bias, bias, bias_s.at[ss], bias_r.at[rs], z_peer(dz)),
            remote(gain, gain, gain_s.at[ss], gain_r.at[rs], z_peer(dz)),
        )

    def b2_send(k, j):
        ref = m_buf.at[head_z(k), y, c, 1]
        return remote(ref, ref, b2_s.at[k, j - 1], b2_r.at[k, j - 1], y_peer(j))

    def b2_recv(k, j):
        ref = m_buf.at[head_z(k), lax.rem(y + NY - j, NY), c, 1]
        return remote(ref, ref, b2_s.at[k, j - 1], b2_r.at[k, j - 1], y_peer(j))

    def c_send(k):
        ref = m_buf.at[head_z(k), :, c]
        return remote(ref, ref, c_s.at[k], c_r.at[k], sibling)

    def c_recv(k):
        ref = m_buf.at[head_z(k), :, 1 - c]
        return remote(ref, ref, c_s.at[k], c_r.at[k], sibling)

    barrier = pltpu.get_barrier_semaphore()
    inbox = (x == INBOX_X) & (c == 0)
    helper = (x == INBOX_X) & (c == 1)

    for j in (1, 2, 3):
        to_inbox = (lax.rem(x + j, NX) == INBOX_X) & (c == 0)
        there = {"sp": x_peer(j)["sp"], "dp": jnp.where(to_inbox, dp + 1, dp)}
        pl.semaphore_signal(barrier, inc=1, device_id=there, device_id_type=MESH)

    @pl.when(inbox)
    def _():
        pl.semaphore_signal(barrier, inc=1, device_id=sibling, device_id_type=MESH)

    for far_z, far_y in [(lax.rem(z + j, NZ), y) for j in (1, NZ - 1)] + [
        (z, lax.rem(y + j, NY)) for j in (1, 2, 3)
    ]:
        pl.semaphore_signal(
            barrier,
            inc=1,
            device_id={"sp": far_z * NX + INBOX_X, "dp": far_y * NC},
            device_id_type=MESH,
        )
    @pl.when(jnp.logical_not(inbox))
    def _():
        pl.semaphore_wait(barrier, jnp.where(helper, 7, 3))

    @pl.when(helper)
    def _():
        pl.semaphore_signal(row_sem, inc=1, device_id=sibling, device_id_type=MESH)

    @pl.when(inbox)
    def _():
        pl.semaphore_wait(row_sem, 1)

    def start_v(k, carry):
        for j in (1, 3, 2):
            v_send(k, j).start()
        return carry

    for j in (1, 2, 3):
        seg_send(j).start()
    lax.fori_loop(0, STEPS, start_v, 0)


    own_a = pltpu.make_async_copy(mix_hbm.at[0, pl.ds(0, HALF)], m_buf.at[z, y, c, 0], loc_sem.at[0])
    own_b = pltpu.make_async_copy(mix_hbm.at[0, pl.ds(HALF, HALF)], m_buf.at[z, y, c, 1], loc_sem.at[1])
    own_bias = pltpu.make_async_copy(bias_hbm, bias_buf.at[z], loc_sem.at[2])
    own_seg = pltpu.make_async_copy(seg_hbm, seg_buf.at[x], loc_sem.at[3])
    own_gate = pltpu.make_async_copy(gate_hbm.at[0], g_buf, loc_sem.at[4])
    own_gain = pltpu.make_async_copy(gain_hbm, gain_buf.at[z], loc_sem.at[5])

    def own_v(k):
        return pltpu.make_async_copy(
            value_hbm.at[0, :, head_cols(k, x)], v_buf.at[k, x_rows(x)], own_v_sem.at[k]
        )

    for own in (own_b, own_a, own_bias, own_gain, own_seg):
        own.start()

    @pl.when(inbox)
    def _():
        pl.semaphore_wait(barrier, 5 * NX * NC)
        for j in range(NX):
            for core in range(NC):
                if j or core:
                    there = {"sp": x_peer(j)["sp"], "dp": y * NC + core}
                    pl.semaphore_signal(far_sem, inc=1, device_id=there, device_id_type=MESH)

    @pl.when(jnp.logical_not(inbox))
    def _():
        pl.semaphore_wait(far_sem, 1)

    def start_own_v(k, carry):
        own_v(k).start()
        return carry

    for j in (1, 2, 3):
        a1_send(j).start()
    own_b.wait()
    b_msg(z, 0, 1, NZ - 1).start()
    b_msg(z, 8, 2, 1).start()
    own_bias.wait()
    own_gain.wait()
    for small in x_msgs(z, 0, 1, NZ - 1) + x_msgs(z, 7, 2, 1):
        small.start()
    for j in (1, 2, 3):
        b2_send(0, j).start()
    lax.fori_loop(0, STEPS, start_own_v, 0)
    own_gate.start()

    own_seg.wait()
    for j in (1, 2, 3):
        seg_recv(j).wait_recv()

    def as_column(row):
        return jnp.transpose(jnp.broadcast_to(row, (HD, row.shape[1])))

    for s in range(NX):
        col_buf[pl.ds(lax.rem(s, 2) * TOK, TOK), :] = as_column(seg_buf[s].astype(F32))
        if s % 2 == 1:
            rows_ids = [seg_buf[s - 1].astype(F32), seg_buf[s].astype(F32)]

            def mask_rows(i, carry):
                rows = pl.ds(pl.multiple_of(i * 64, 64), 64)
                ids = col_buf[rows, :]
                for half in range(2):
                    for t in range(TOK // HD):
                        there = rows_ids[half][:, t * HD : (t + 1) * HD]
                        mask_buf[s // 2, rows, half * TOK + t * HD : half * TOK + (t + 1) * HD] = jnp.where(
                            ids == there, 1.0, 0.0
                        ).astype(BF16)
                return carry

            lax.fori_loop(0, BLK // 64, mask_rows, 0)

    def ways(k):
        return NZ - 1 if k % 2 else 1

    def serve_second(k):
        zh = head_z(k)
        for small in x_msgs(zh, k, k, 1):
            small.wait_recv()
        if k < 7:
            b_msg(zh, k, k, 1).wait_recv()
        else:
            b_half(zh, 0, 7, 7, 1).wait_recv()
            b_half(zh, HALF // 2, 7, 8, 1).wait_recv()
        if k <= 4:
            b_msg(zh, k, k + 2, ways(k)).start()
        elif k == 5:
            b_half(zh, 0, 5, 7, ways(k)).start()
        elif k == 6:
            b_half(zh, HALF // 2, 6, 8, ways(k)).start()
        if k <= 5:
            for small in x_msgs(zh, k, k + 2, ways(k)):
                small.start()
        for j in (1, 2, 3):
            b2_send(k, j).start()

    def serve_first(k, half):
        zh = head_z(k)
        a_msg(zh, half, 0, 2 * k + half, 1).wait_recv()
        if k <= 4 or k == 5 + half:
            to = 2 * (k + 2) + half if k <= 4 else 14 + half
            a_msg(zh, half, 2 * k + half, to, ways(k)).start()

    def across(k):
        for j in (1, 2, 3):
            b2_recv(k, j).wait_recv()
        c_send(k).start()

    for k in (1, 2):
        serve_second(k)
    own_a.wait()
    for j in (1, 2, 3):
        a1_recv(j).wait_recv()
    for half in (0, 1):
        a_msg(z, half, half, 2 + half, NZ - 1).start()
        a_msg(z, half, 14 + half, 4 + half, 1).start()
    for k in (3, 4, 5, 6):
        serve_second(k)
    across(0)
    serve_second(7)

    def compute(k):
        zh = head_z(k)
        for pair in (2, 3):

            @pl.when(k == 2 * pair - 2)
            def _():
                serve_first(2 * pair - 1, 0)
                serve_first(2 * pair, 0)

        own_v(k).wait()
        for j in (1, 2, 3):
            v_recv(k, j).wait_recv()
        gain = gain_buf[zh].astype(F32)
        bias = bias_buf[zh].astype(F32)
        for t in range(BLK // TOK):
            col_buf[pl.ds(t * TOK, TOK), :] = as_column(bias[:, t * TOK : (t + 1) * TOK])

        def norm_rows(i, carry):
            rows = pl.ds(pl.multiple_of(i * 128, 128), 128)
            act = gelu(v_buf[k, rows, :].astype(F32))
            scaled = act * lax.rsqrt(jnp.mean(act * act, axis=-1, keepdims=True) + EPSILON)
            vn_buf[rows, :] = (scaled * gain).astype(BF16)
            return carry

        lax.fori_loop(0, NX * TOK // 128, norm_rows, 0)

        @pl.when(k == 0)
        def _():
            serve_first(1, 0)
            serve_first(2, 0)

        c_recv(k).wait_recv()

        def mix_rows(i, carry):
            block, part = i // NY, lax.rem(i, NY)
            rows = pl.ds(pl.multiple_of(part * 256, 256), 256)
            matrix = m_buf[zh, part].reshape(256, BLK) * mask_buf[block, rows, :]
            values = vn_buf[pl.ds(pl.multiple_of(block * BLK, BLK), BLK), :]
            summed = jnp.dot(matrix, values, preferred_element_type=F32)
            r_buf[k, pl.ds(pl.multiple_of(block * BLK + part * 256, 256), 256), :] = (
                summed + col_buf[rows, :]
            ).astype(BF16)
            return carry

        lax.fori_loop(0, 2 * NY, mix_rows, 0)
        for j in (1, 3, 2):
            r_send(k, j).start()

    def step(k, carry):
        compute(k)
        for pair in (1, 2, 3):

            @pl.when(k == 2 * pair - 2)
            def _():
                serve_first(2 * pair - 1, 1)
                serve_first(2 * pair, 1)
                across(2 * pair - 1)
                across(2 * pair)

        @pl.when(k == 5)
        def _():
            serve_first(7, 0)
            serve_first(7, 1)
            across(7)

        return carry

    lax.fori_loop(0, STEPS, step, 0)

    def sent(k, carry):
        for j in (1, 2, 3):
            v_send(k, j).wait_send()
            b2_send(k, j).wait_send()
        c_send(k).wait_send()
        return carry

    lax.fori_loop(0, STEPS, sent, 0)
    for j in (1, 2, 3):
        seg_send(j).wait_send()
        a1_send(j).wait_send()
    for k in (0, 1, 2, 3, 4, 5, 6, 7, 8, 9, 10, 13, 14, 15):
        a_msg(z, 0, k, 0, 1).wait_send()
    for k in (0, 1, 2, 3, 4, 8):
        b_msg(z, k, 0, 1).wait_send()
    for k in (5, 6):
        b_half(z, 0, k, 0, 1).wait_send()
    for k in (0, 1, 2, 3, 4, 5, 7):
        for small in x_msgs(z, k, 0, 1):
            small.wait_send()

    own_gate.wait()

    def gate_rows(k, xs, source):
        cols = head_cols(k, xs)
        for i in range(TOK // 128):
            rows = pl.ds(i * 128, 128)
            gate = gelu(g_buf[rows, cols].astype(F32))
            out_ref[0, rows, cols] = (gate * source(i * 128).astype(F32)).astype(BF16)

    def own_gated(k, carry):
        gate_rows(
            k, x, lambda lo: r_buf[k, pl.ds(pl.multiple_of(x * TOK + lo, 128), 128), :]
        )
        return carry

    lax.fori_loop(0, STEPS, own_gated, 0)

    def gated(k, carry):
        for j in (1, 3, 2):
            r_recv(k, j).wait_recv()
            xs = lax.rem(x + NX - j, NX)
            gate_rows(k, xs, lambda lo: o_buf[xs, k, pl.ds(lo, 128), :])
        for j in (1, 3, 2):
            r_send(k, j).wait_send()
        return carry

    lax.fori_loop(0, STEPS, gated, 0)


def per_device(gate_in, value_in, segments, value_gain, mixing, mixing_bias):
    any_space = pl.BlockSpec(memory_space=pl.ANY)
    dma = pltpu.SemaphoreType.DMA
    return pl.pallas_call(
        kernel,
        out_shape=pltpu.VMEM(value_in.shape, BF16),
        in_specs=[any_space] * 6,
        out_specs=pl.BlockSpec(memory_space=pltpu.VMEM),
        scratch_shapes=[
            pltpu.VMEM((NZ, NY, NC, 2, HALF, BLK), BF16),
            pltpu.VMEM((STEPS, NX * TOK, HD), BF16),
            pltpu.VMEM((STEPS, NX * TOK, HD), BF16),
            pltpu.VMEM((NX, STEPS, TOK, HD), BF16),
            pltpu.VMEM((TOK, NX * NZ * HD), BF16),
            pltpu.VMEM((2, BLK, BLK), BF16),
            pltpu.VMEM((NX * TOK, HD), BF16),
            pltpu.VMEM((BLK, HD), F32),
            pltpu.VMEM((NX, 1, TOK), jnp.int32),
            pltpu.VMEM((NZ, 1, BLK), BF16),
            pltpu.VMEM((NZ, 1, HD), BF16),
            dma((6,)),
            dma((STEPS,)),
            dma((3,)),
            dma((3,)),
            dma((STEPS, 3)),
            dma((STEPS, 3)),
            dma((STEPS, 3)),
            dma((STEPS, 3)),
            dma((3,)),
            dma((3,)),
            dma((16,)),
            dma((16,)),
            dma((9,)),
            dma((9,)),
            dma((8,)),
            dma((8,)),
            dma((8,)),
            dma((8,)),
            dma((STEPS, 3)),
            dma((STEPS, 3)),
            dma((STEPS,)),
            dma((STEPS,)),
            pltpu.SemaphoreType.REGULAR,
            pltpu.SemaphoreType.REGULAR,
        ],
        compiler_params=pltpu.CompilerParams(
            collective_id=0, has_side_effects=True, vmem_limit_bytes=48 * 1024 * 1024
        ),
    )(*(pltpu.with_memory_space_constraint(a, pltpu.HBM) for a in (gate_in, value_in, segments, value_gain.reshape(1, HD), mixing, mixing_bias)))


def solution(mesh):
    return jax.shard_map(
        per_device,
        mesh=mesh,
        in_specs=(
            P("dp", "sp", None),
            P("dp", "sp", None),
            P("dp", "sp"),
            P("sp"),
            P("sp", "dp", None),
            P("sp", None),
        ),
        out_specs=P("dp", "sp", None),
        check_vma=False,
    )
```

```python
import jax
import jax.numpy as jnp
from jax import lax
from jax.experimental import pallas as pl
from jax.experimental.pallas import tpu as pltpu
from jax.sharding import PartitionSpec as P

MESH = pl.DeviceIdType.MESH
EPSILON = 1e-06
BF16, F32 = jnp.bfloat16, jnp.float32
NX, NY, NZ, NC = 4, 4, 8, 2
HD = 128
TOK = 512
BLK = 1024
HALF = 64
STEPS = 8
INBOX_X = 0


def gelu(x):
    inner = 0.7978845608028654 * (x + 0.044715 * (x * x * x))
    return x * (0.5 * (1.0 + jnp.tanh(inner)))


def kernel(
    gate_hbm,
    value_hbm,
    seg_hbm,
    gain_hbm,
    mix_hbm,
    bias_hbm,
    out_ref,
    m_buf,
    v_buf,
    r_buf,
    o_buf,
    g_buf,
    mask_buf,
    vn_buf,
    col_buf,
    seg_buf,
    bias_buf,
    gain_buf,
    loc_sem,
    own_v_sem,
    seg_s,
    seg_r,
    v_s,
    v_r,
    r_s,
    r_r,
    a1_s,
    a1_r,
    a_s,
    a_r,
    b_s,
    b_r,
    bias_s,
    bias_r,
    gain_s,
    gain_r,
    b2_s,
    b2_r,
    c_s,
    c_r,
    row_sem,
    far_sem,
):
    sp, dp = lax.axis_index("sp"), lax.axis_index("dp")
    z, x = sp // NX, lax.rem(sp, NX)
    y, c = dp // NC, lax.rem(dp, NC)

    def x_peer(j):
        return {"sp": z * NX + lax.rem(x + j, NX), "dp": dp}

    def y_peer(j):
        return {"sp": sp, "dp": lax.rem(y + j, NY) * NC + c}

    def z_peer(j):
        return {"sp": lax.rem(z + j, NZ) * NX + x, "dp": dp}

    sibling = {"sp": sp, "dp": y * NC + (1 - c)}

    def remote(src, dst, ss, rs, dev):
        return pltpu.make_async_remote_copy(
            src_ref=src, dst_ref=dst, send_sem=ss, recv_sem=rs, device_id=dev, device_id_type=MESH
        )

    def head_z(k):
        far = (k + 1) // 2
        return lax.rem(z + jnp.where(lax.rem(k, 2) == 1, far, NZ - far), NZ)

    def head_cols(k, xs):
        return pl.ds(pl.multiple_of((head_z(k) * NX + xs) * HD, HD), HD)

    def x_rows(xs):
        return pl.ds(pl.multiple_of(xs * TOK, TOK), TOK)

    def v_send(k, j):
        xs = lax.rem(x + j, NX)
        return remote(
            value_hbm.at[0, :, head_cols(k, xs)],
            v_buf.at[k, x_rows(x)],
            v_s.at[k, j - 1],
            v_r.at[k, j - 1],
            x_peer(j),
        )

    def v_recv(k, j):
        xs = lax.rem(x + NX - j, NX)
        return remote(
            v_buf.at[k, x_rows(xs)], v_buf.at[k, x_rows(xs)], v_s.at[k, j - 1], v_r.at[k, j - 1], x_peer(j)
        )

    def r_send(k, j):
        xs = lax.rem(x + j, NX)
        return remote(
            r_buf.at[k, x_rows(xs)], o_buf.at[x, k], r_s.at[k, j - 1], r_r.at[k, j - 1], x_peer(j)
        )

    def r_recv(k, j):
        xs = lax.rem(x + NX - j, NX)
        return remote(o_buf.at[xs, k], o_buf.at[xs, k], r_s.at[k, j - 1], r_r.at[k, j - 1], x_peer(j))

    def seg_send(j):
        return remote(seg_hbm, seg_buf.at[x], seg_s.at[j - 1], seg_r.at[j - 1], x_peer(j))

    def seg_recv(j):
        xs = lax.rem(x + NX - j, NX)
        return remote(seg_buf.at[xs], seg_buf.at[xs], seg_s.at[j - 1], seg_r.at[j - 1], x_peer(j))

    def a1_send(j):
        return remote(
            mix_hbm.at[0, pl.ds(0, HALF)], m_buf.at[z, y, c, 0], a1_s.at[j - 1], a1_r.at[j - 1], y_peer(j)
        )

    def a1_recv(j):
        ref = m_buf.at[z, lax.rem(y + NY - j, NY), c, 0]
        return remote(ref, ref, a1_s.at[j - 1], a1_r.at[j - 1], y_peer(j))

    def a_msg(zh, half, ss, rs, dz):
        ref = m_buf.at[zh, pl.ds(2 * half, 2), c, 0]
        return remote(ref, ref, a_s.at[ss], a_r.at[rs], z_peer(dz))

    def b_msg(zh, ss, rs, dz):
        ref = m_buf.at[zh, y, c, 1]
        return remote(ref, ref, b_s.at[ss], b_r.at[rs], z_peer(dz))

    def b_half(zh, lo, ss, rs, dz):
        ref = m_buf.at[zh, y, c, 1, pl.ds(lo, HALF // 2)]
        return remote(ref, ref, b_s.at[ss], b_r.at[rs], z_peer(dz))

    def x_msgs(zh, ss, rs, dz):
        bias, gain = bias_buf.at[zh], gain_buf.at[zh]
        return (
            remote(bias, bias, bias_s.at[ss], bias_r.at[rs], z_peer(dz)),
            remote(gain, gain, gain_s.at[ss], gain_r.at[rs], z_peer(dz)),
        )

    def b2_send(k, j):
        ref = m_buf.at[head_z(k), y, c, 1]
        return remote(ref, ref, b2_s.at[k, j - 1], b2_r.at[k, j - 1], y_peer(j))

    def b2_recv(k, j):
        ref = m_buf.at[head_z(k), lax.rem(y + NY - j, NY), c, 1]
        return remote(ref, ref, b2_s.at[k, j - 1], b2_r.at[k, j - 1], y_peer(j))

    def c_send(k):
        ref = m_buf.at[head_z(k), :, c]
        return remote(ref, ref, c_s.at[k], c_r.at[k], sibling)

    def c_recv(k):
        ref = m_buf.at[head_z(k), :, 1 - c]
        return remote(ref, ref, c_s.at[k], c_r.at[k], sibling)

    barrier = pltpu.get_barrier_semaphore()
    inbox = (x == INBOX_X) & (c == 0)
    helper = (x == INBOX_X) & (c == 1)

    for j in (1, 2, 3):
        to_inbox = (lax.rem(x + j, NX) == INBOX_X) & (c == 0)
        there = {"sp": x_peer(j)["sp"], "dp": jnp.where(to_inbox, dp + 1, dp)}
        pl.semaphore_signal(barrier, inc=1, device_id=there, device_id_type=MESH)

    @pl.when(inbox)
    def _():
        pl.semaphore_signal(barrier, inc=1, device_id=sibling, device_id_type=MESH)

    for far_z, far_y in [(lax.rem(z + j, NZ), y) for j in (1, NZ - 1)] + [
        (z, lax.rem(y + j, NY)) for j in (1, 2, 3)
    ]:
        pl.semaphore_signal(
            barrier,
            inc=1,
            device_id={"sp": far_z * NX + INBOX_X, "dp": far_y * NC},
            device_id_type=MESH,
        )
    @pl.when(jnp.logical_not(inbox))
    def _():
        pl.semaphore_wait(barrier, jnp.where(helper, 7, 3))

    @pl.when(helper)
    def _():
        pl.semaphore_signal(row_sem, inc=1, device_id=sibling, device_id_type=MESH)

    @pl.when(inbox)
    def _():
        pl.semaphore_wait(row_sem, 1)

    def start_v(k, carry):
        for j in (1, 3):
            v_send(k, j).start()
        return carry

    for j in (1, 2, 3):
        seg_send(j).start()
    def start_far_v(k, carry):
        v_send(k, 2).start()
        return carry

    lax.fori_loop(0, 2, start_far_v, 0)
    lax.fori_loop(0, 1, start_v, 0)
    lax.fori_loop(2, STEPS, start_far_v, 0)
    lax.fori_loop(1, STEPS, start_v, 0)


    own_a = pltpu.make_async_copy(mix_hbm.at[0, pl.ds(0, HALF)], m_buf.at[z, y, c, 0], loc_sem.at[0])
    own_b = pltpu.make_async_copy(mix_hbm.at[0, pl.ds(HALF, HALF)], m_buf.at[z, y, c, 1], loc_sem.at[1])
    own_bias = pltpu.make_async_copy(bias_hbm, bias_buf.at[z], loc_sem.at[2])
    own_seg = pltpu.make_async_copy(seg_hbm, seg_buf.at[x], loc_sem.at[3])
    own_gate = pltpu.make_async_copy(gate_hbm.at[0], g_buf, loc_sem.at[4])
    own_gain = pltpu.make_async_copy(gain_hbm, gain_buf.at[z], loc_sem.at[5])

    def own_v(k):
        return pltpu.make_async_copy(
            value_hbm.at[0, :, head_cols(k, x)], v_buf.at[k, x_rows(x)], own_v_sem.at[k]
        )

    for own in (own_b, own_a, own_bias, own_gain, own_seg):
        own.start()

    @pl.when(inbox)
    def _():
        pl.semaphore_wait(barrier, 5 * NX * NC)
        for j in range(NX):
            for core in range(NC):
                if j or core:
                    there = {"sp": x_peer(j)["sp"], "dp": y * NC + core}
                    pl.semaphore_signal(far_sem, inc=1, device_id=there, device_id_type=MESH)

    @pl.when(jnp.logical_not(inbox))
    def _():
        pl.semaphore_wait(far_sem, 1)

    def start_own_v(k, carry):
        own_v(k).start()
        return carry

    for j in (1, 2, 3):
        a1_send(j).start()
    own_b.wait()
    b_msg(z, 0, 1, NZ - 1).start()
    b_msg(z, 8, 2, 1).start()
    own_bias.wait()
    own_gain.wait()
    for small in x_msgs(z, 0, 1, NZ - 1) + x_msgs(z, 7, 2, 1):
        small.start()
    for j in (1, 2, 3):
        b2_send(0, j).start()
    lax.fori_loop(0, STEPS, start_own_v, 0)
    own_gate.start()

    own_seg.wait()
    for j in (1, 2, 3):
        seg_recv(j).wait_recv()

    def as_column(row):
        return jnp.transpose(jnp.broadcast_to(row, (HD, row.shape[1])))

    for s in range(NX):
        col_buf[pl.ds(lax.rem(s, 2) * TOK, TOK), :] = as_column(seg_buf[s].astype(F32))
        if s % 2 == 1:
            rows_ids = [seg_buf[s - 1].astype(F32), seg_buf[s].astype(F32)]

            def mask_rows(i, carry):
                rows = pl.ds(pl.multiple_of(i * 64, 64), 64)
                ids = col_buf[rows, :]
                for half in range(2):
                    for t in range(TOK // HD):
                        there = rows_ids[half][:, t * HD : (t + 1) * HD]
                        mask_buf[s // 2, rows, half * TOK + t * HD : half * TOK + (t + 1) * HD] = jnp.where(
                            ids == there, 1.0, 0.0
                        ).astype(BF16)
                return carry

            lax.fori_loop(0, BLK // 64, mask_rows, 0)

    def ways(k):
        return NZ - 1 if k % 2 else 1

    def serve_second(k):
        zh = head_z(k)
        for small in x_msgs(zh, k, k, 1):
            small.wait_recv()
        if k < 7:
            b_msg(zh, k, k, 1).wait_recv()
        else:
            b_half(zh, 0, 7, 7, 1).wait_recv()
            b_half(zh, HALF // 2, 7, 8, 1).wait_recv()
        if k <= 4:
            b_msg(zh, k, k + 2, ways(k)).start()
        elif k == 5:
            b_half(zh, 0, 5, 7, ways(k)).start()
        elif k == 6:
            b_half(zh, HALF // 2, 6, 8, ways(k)).start()
        if k <= 5:
            for small in x_msgs(zh, k, k + 2, ways(k)):
                small.start()
        for j in (1, 2, 3):
            b2_send(k, j).start()

    def serve_first(k, half):
        zh = head_z(k)
        a_msg(zh, half, 0, 2 * k + half, 1).wait_recv()
        if k <= 4 or k == 5 + half:
            to = 2 * (k + 2) + half if k <= 4 else 14 + half
            a_msg(zh, half, 2 * k + half, to, ways(k)).start()

    def across(k):
        for j in (1, 2, 3):
            b2_recv(k, j).wait_recv()
        c_send(k).start()

    for k in (1, 2):
        serve_second(k)
    own_a.wait()
    for j in (1, 2, 3):
        a1_recv(j).wait_recv()
    for half in (0, 1):
        a_msg(z, half, half, 2 + half, NZ - 1).start()
        a_msg(z, half, 14 + half, 4 + half, 1).start()
    for k in (3, 4, 5, 6):
        serve_second(k)
    across(0)
    serve_second(7)

    def compute(k):
        zh = head_z(k)
        for pair in (2, 3):

            @pl.when(k == 2 * pair - 2)
            def _():
                serve_first(2 * pair - 1, 0)
                serve_first(2 * pair, 0)

        own_v(k).wait()
        for j in (1, 2, 3):
            v_recv(k, j).wait_recv()
        gain = gain_buf[zh].astype(F32)
        bias = bias_buf[zh].astype(F32)
        for t in range(BLK // TOK):
            col_buf[pl.ds(t * TOK, TOK), :] = as_column(bias[:, t * TOK : (t + 1) * TOK])

        def norm_rows(i, carry):
            rows = pl.ds(pl.multiple_of(i * 128, 128), 128)
            act = gelu(v_buf[k, rows, :].astype(F32))
            scaled = act * lax.rsqrt(jnp.mean(act * act, axis=-1, keepdims=True) + EPSILON)
            vn_buf[rows, :] = (scaled * gain).astype(BF16)
            return carry

        lax.fori_loop(0, NX * TOK // 128, norm_rows, 0)

        @pl.when(k == 0)
        def _():
            serve_first(1, 0)
            serve_first(2, 0)

        c_recv(k).wait_recv()

        def mix_rows(i, carry):
            block, part = i // NY, lax.rem(i, NY)
            rows = pl.ds(pl.multiple_of(part * 256, 256), 256)
            matrix = m_buf[zh, part].reshape(256, BLK) * mask_buf[block, rows, :]
            values = vn_buf[pl.ds(pl.multiple_of(block * BLK, BLK), BLK), :]
            summed = jnp.dot(matrix, values, preferred_element_type=F32)
            r_buf[k, pl.ds(pl.multiple_of(block * BLK + part * 256, 256), 256), :] = (
                summed + col_buf[rows, :]
            ).astype(BF16)
            return carry

        lax.fori_loop(0, 2 * NY, mix_rows, 0)
        for j in (1, 3, 2):
            r_send(k, j).start()

    def step(k, carry):
        compute(k)
        for pair in (1, 2, 3):

            @pl.when(k == 2 * pair - 2)
            def _():
                serve_first(2 * pair - 1, 1)
                serve_first(2 * pair, 1)
                across(2 * pair - 1)
                across(2 * pair)

        @pl.when(k == 5)
        def _():
            serve_first(7, 0)
            serve_first(7, 1)
            across(7)

        return carry

    lax.fori_loop(0, STEPS, step, 0)

    def sent(k, carry):
        for j in (1, 2, 3):
            v_send(k, j).wait_send()
            b2_send(k, j).wait_send()
        c_send(k).wait_send()
        return carry

    lax.fori_loop(0, STEPS, sent, 0)
    for j in (1, 2, 3):
        seg_send(j).wait_send()
        a1_send(j).wait_send()
    for k in (0, 1, 2, 3, 4, 5, 6, 7, 8, 9, 10, 13, 14, 15):
        a_msg(z, 0, k, 0, 1).wait_send()
    for k in (0, 1, 2, 3, 4, 8):
        b_msg(z, k, 0, 1).wait_send()
    for k in (5, 6):
        b_half(z, 0, k, 0, 1).wait_send()
    for k in (0, 1, 2, 3, 4, 5, 7):
        for small in x_msgs(z, k, 0, 1):
            small.wait_send()

    own_gate.wait()

    def gate_rows(k, xs, source):
        cols = head_cols(k, xs)
        for i in range(TOK // 128):
            rows = pl.ds(i * 128, 128)
            gate = gelu(g_buf[rows, cols].astype(F32))
            out_ref[0, rows, cols] = (gate * source(i * 128).astype(F32)).astype(BF16)

    def own_gated(k, carry):
        gate_rows(
            k, x, lambda lo: r_buf[k, pl.ds(pl.multiple_of(x * TOK + lo, 128), 128), :]
        )
        return carry

    lax.fori_loop(0, STEPS, own_gated, 0)

    def gated(k, carry):
        for j in (1, 3, 2):
            r_recv(k, j).wait_recv()
            xs = lax.rem(x + NX - j, NX)
            gate_rows(k, xs, lambda lo: o_buf[xs, k, pl.ds(lo, 128), :])
        for j in (1, 3, 2):
            r_send(k, j).wait_send()
        return carry

    lax.fori_loop(0, STEPS, gated, 0)


def per_device(gate_in, value_in, segments, value_gain, mixing, mixing_bias):
    any_space = pl.BlockSpec(memory_space=pl.ANY)
    dma = pltpu.SemaphoreType.DMA
    return pl.pallas_call(
        kernel,
        out_shape=pltpu.VMEM(value_in.shape, BF16),
        in_specs=[any_space] * 6,
        out_specs=pl.BlockSpec(memory_space=pltpu.VMEM),
        scratch_shapes=[
            pltpu.VMEM((NZ, NY, NC, 2, HALF, BLK), BF16),
            pltpu.VMEM((STEPS, NX * TOK, HD), BF16),
            pltpu.VMEM((STEPS, NX * TOK, HD), BF16),
            pltpu.VMEM((NX, STEPS, TOK, HD), BF16),
            pltpu.VMEM((TOK, NX * NZ * HD), BF16),
            pltpu.VMEM((2, BLK, BLK), BF16),
            pltpu.VMEM((NX * TOK, HD), BF16),
            pltpu.VMEM((BLK, HD), F32),
            pltpu.VMEM((NX, 1, TOK), jnp.int32),
            pltpu.VMEM((NZ, 1, BLK), BF16),
            pltpu.VMEM((NZ, 1, HD), BF16),
            dma((6,)),
            dma((STEPS,)),
            dma((3,)),
            dma((3,)),
            dma((STEPS, 3)),
            dma((STEPS, 3)),
            dma((STEPS, 3)),
            dma((STEPS, 3)),
            dma((3,)),
            dma((3,)),
            dma((16,)),
            dma((16,)),
            dma((9,)),
            dma((9,)),
            dma((8,)),
            dma((8,)),
            dma((8,)),
            dma((8,)),
            dma((STEPS, 3)),
            dma((STEPS, 3)),
            dma((STEPS,)),
            dma((STEPS,)),
            pltpu.SemaphoreType.REGULAR,
            pltpu.SemaphoreType.REGULAR,
        ],
        compiler_params=pltpu.CompilerParams(
            collective_id=0, has_side_effects=True, vmem_limit_bytes=48 * 1024 * 1024
        ),
    )(*(pltpu.with_memory_space_constraint(a, pltpu.HBM) for a in (gate_in, value_in, segments, value_gain.reshape(1, HD), mixing, mixing_bias)))


def solution(mesh):
    return jax.shard_map(
        per_device,
        mesh=mesh,
        in_specs=(
            P("dp", "sp", None),
            P("dp", "sp", None),
            P("dp", "sp"),
            P("sp"),
            P("sp", "dp", None),
            P("sp", None),
        ),
        out_specs=P("dp", "sp", None),
        check_vma=False,
    )
```

```python
import jax
import jax.numpy as jnp
from jax import lax
from jax.experimental import pallas as pl
from jax.experimental.pallas import tpu as pltpu
from jax.sharding import PartitionSpec as P

MESH = pl.DeviceIdType.MESH
EPSILON = 1e-06
BF16, F32 = jnp.bfloat16, jnp.float32
NX, NY, NZ, NC = 4, 4, 8, 2
HD = 128
TOK = 512
BLK = 1024
HALF = 64
STEPS = 8
INBOX_X = 0


def gelu(x):
    inner = 0.7978845608028654 * (x + 0.044715 * (x * x * x))
    return x * (0.5 * (1.0 + jnp.tanh(inner)))


def kernel(
    gate_hbm,
    value_hbm,
    seg_hbm,
    gain_hbm,
    mix_hbm,
    bias_hbm,
    out_ref,
    m_buf,
    v_buf,
    r_buf,
    o_buf,
    g_buf,
    mask_buf,
    vn_buf,
    col_buf,
    seg_buf,
    bias_buf,
    gain_buf,
    loc_sem,
    own_v_sem,
    seg_s,
    seg_r,
    v_s,
    v_r,
    r_s,
    r_r,
    a1_s,
    a1_r,
    a_s,
    a_r,
    b_s,
    b_r,
    bias_s,
    bias_r,
    gain_s,
    gain_r,
    b2_s,
    b2_r,
    c_s,
    c_r,
    row_sem,
    far_sem,
):
    sp, dp = lax.axis_index("sp"), lax.axis_index("dp")
    z, x = sp // NX, lax.rem(sp, NX)
    y, c = dp // NC, lax.rem(dp, NC)

    def x_peer(j):
        return {"sp": z * NX + lax.rem(x + j, NX), "dp": dp}

    def y_peer(j):
        return {"sp": sp, "dp": lax.rem(y + j, NY) * NC + c}

    def z_peer(j):
        return {"sp": lax.rem(z + j, NZ) * NX + x, "dp": dp}

    sibling = {"sp": sp, "dp": y * NC + (1 - c)}

    def remote(src, dst, ss, rs, dev):
        return pltpu.make_async_remote_copy(
            src_ref=src, dst_ref=dst, send_sem=ss, recv_sem=rs, device_id=dev, device_id_type=MESH
        )

    def head_z(k):
        far = (k + 1) // 2
        return lax.rem(z + jnp.where(lax.rem(k, 2) == 1, far, NZ - far), NZ)

    def head_cols(k, xs):
        return pl.ds(pl.multiple_of((head_z(k) * NX + xs) * HD, HD), HD)

    def x_rows(xs):
        return pl.ds(pl.multiple_of(xs * TOK, TOK), TOK)

    def v_send(k, j):
        xs = lax.rem(x + j, NX)
        return remote(
            value_hbm.at[0, :, head_cols(k, xs)],
            v_buf.at[k, x_rows(x)],
            v_s.at[k, j - 1],
            v_r.at[k, j - 1],
            x_peer(j),
        )

    def v_recv(k, j):
        xs = lax.rem(x + NX - j, NX)
        return remote(
            v_buf.at[k, x_rows(xs)], v_buf.at[k, x_rows(xs)], v_s.at[k, j - 1], v_r.at[k, j - 1], x_peer(j)
        )

    def r_send(k, j):
        xs = lax.rem(x + j, NX)
        return remote(
            r_buf.at[k, x_rows(xs)], o_buf.at[x, k], r_s.at[k, j - 1], r_r.at[k, j - 1], x_peer(j)
        )

    def r_recv(k, j):
        xs = lax.rem(x + NX - j, NX)
        return remote(o_buf.at[xs, k], o_buf.at[xs, k], r_s.at[k, j - 1], r_r.at[k, j - 1], x_peer(j))

    def seg_send(j):
        return remote(seg_hbm, seg_buf.at[x], seg_s.at[j - 1], seg_r.at[j - 1], x_peer(j))

    def seg_recv(j):
        xs = lax.rem(x + NX - j, NX)
        return remote(seg_buf.at[xs], seg_buf.at[xs], seg_s.at[j - 1], seg_r.at[j - 1], x_peer(j))

    def a1_send(j):
        return remote(
            mix_hbm.at[0, pl.ds(0, HALF)], m_buf.at[z, y, c, 0], a1_s.at[j - 1], a1_r.at[j - 1], y_peer(j)
        )

    def a1_recv(j):
        ref = m_buf.at[z, lax.rem(y + NY - j, NY), c, 0]
        return remote(ref, ref, a1_s.at[j - 1], a1_r.at[j - 1], y_peer(j))

    def a_msg(zh, half, ss, rs, dz):
        ref = m_buf.at[zh, pl.ds(2 * half, 2), c, 0]
        return remote(ref, ref, a_s.at[ss], a_r.at[rs], z_peer(dz))

    def b_msg(zh, ss, rs, dz):
        ref = m_buf.at[zh, y, c, 1]
        return remote(ref, ref, b_s.at[ss], b_r.at[rs], z_peer(dz))

    def b_half(zh, lo, ss, rs, dz):
        ref = m_buf.at[zh, y, c, 1, pl.ds(lo, HALF // 2)]
        return remote(ref, ref, b_s.at[ss], b_r.at[rs], z_peer(dz))

    def x_msgs(zh, ss, rs, dz):
        bias, gain = bias_buf.at[zh], gain_buf.at[zh]
        return (
            remote(bias, bias, bias_s.at[ss], bias_r.at[rs], z_peer(dz)),
            remote(gain, gain, gain_s.at[ss], gain_r.at[rs], z_peer(dz)),
        )

    def b2_send(k, j):
        ref = m_buf.at[head_z(k), y, c, 1]
        return remote(ref, ref, b2_s.at[k, j - 1], b2_r.at[k, j - 1], y_peer(j))

    def b2_recv(k, j):
        ref = m_buf.at[head_z(k), lax.rem(y + NY - j, NY), c, 1]
        return remote(ref, ref, b2_s.at[k, j - 1], b2_r.at[k, j - 1], y_peer(j))

    def c_send(k):
        ref = m_buf.at[head_z(k), :, c]
        return remote(ref, ref, c_s.at[k], c_r.at[k], sibling)

    def c_recv(k):
        ref = m_buf.at[head_z(k), :, 1 - c]
        return remote(ref, ref, c_s.at[k], c_r.at[k], sibling)

    barrier = pltpu.get_barrier_semaphore()
    inbox = (x == INBOX_X) & (c == 0)
    helper = (x == INBOX_X) & (c == 1)

    for j in (1, 2, 3):
        to_inbox = (lax.rem(x + j, NX) == INBOX_X) & (c == 0)
        there = {"sp": x_peer(j)["sp"], "dp": jnp.where(to_inbox, dp + 1, dp)}
        pl.semaphore_signal(barrier, inc=1, device_id=there, device_id_type=MESH)

    @pl.when(inbox)
    def _():
        pl.semaphore_signal(barrier, inc=1, device_id=sibling, device_id_type=MESH)

    for far_z, far_y in [(lax.rem(z + j, NZ), y) for j in (1, NZ - 1)] + [
        (z, lax.rem(y + j, NY)) for j in (1, 2, 3)
    ]:
        pl.semaphore_signal(
            barrier,
            inc=1,
            device_id={"sp": far_z * NX + INBOX_X, "dp": far_y * NC},
            device_id_type=MESH,
        )
    @pl.when(jnp.logical_not(inbox))
    def _():
        pl.semaphore_wait(barrier, jnp.where(helper, 7, 3))

    @pl.when(helper)
    def _():
        pl.semaphore_signal(row_sem, inc=1, device_id=sibling, device_id_type=MESH)

    @pl.when(inbox)
    def _():
        pl.semaphore_wait(row_sem, 1)

    def start_v(k, carry):
        for j in (1, 3):
            v_send(k, j).start()
        return carry

    for j in (1, 2, 3):
        seg_send(j).start()
    def start_far_v(k, carry):
        v_send(k, 2).start()
        return carry

    lax.fori_loop(0, 2, start_far_v, 0)
    lax.fori_loop(0, 1, start_v, 0)
    lax.fori_loop(2, 5, start_far_v, 0)
    lax.fori_loop(1, 2, start_v, 0)
    lax.fori_loop(5, STEPS, start_far_v, 0)
    lax.fori_loop(2, STEPS, start_v, 0)


    own_a = pltpu.make_async_copy(mix_hbm.at[0, pl.ds(0, HALF)], m_buf.at[z, y, c, 0], loc_sem.at[0])
    own_b = pltpu.make_async_copy(mix_hbm.at[0, pl.ds(HALF, HALF)], m_buf.at[z, y, c, 1], loc_sem.at[1])
    own_bias = pltpu.make_async_copy(bias_hbm, bias_buf.at[z], loc_sem.at[2])
    own_seg = pltpu.make_async_copy(seg_hbm, seg_buf.at[x], loc_sem.at[3])
    own_gate = pltpu.make_async_copy(gate_hbm.at[0], g_buf, loc_sem.at[4])
    own_gain = pltpu.make_async_copy(gain_hbm, gain_buf.at[z], loc_sem.at[5])

    def own_v(k):
        return pltpu.make_async_copy(
            value_hbm.at[0, :, head_cols(k, x)], v_buf.at[k, x_rows(x)], own_v_sem.at[k]
        )

    for own in (own_b, own_a, own_bias, own_gain, own_seg):
        own.start()

    @pl.when(inbox)
    def _():
        pl.semaphore_wait(barrier, 5 * NX * NC)
        for j in range(NX):
            for core in range(NC):
                if j or core:
                    there = {"sp": x_peer(j)["sp"], "dp": y * NC + core}
                    pl.semaphore_signal(far_sem, inc=1, device_id=there, device_id_type=MESH)

    @pl.when(jnp.logical_not(inbox))
    def _():
        pl.semaphore_wait(far_sem, 1)

    def start_own_v(k, carry):
        own_v(k).start()
        return carry

    for j in (1, 2, 3):
        a1_send(j).start()
    own_b.wait()
    b_msg(z, 0, 1, NZ - 1).start()
    b_msg(z, 8, 2, 1).start()
    own_bias.wait()
    own_gain.wait()
    for small in x_msgs(z, 0, 1, NZ - 1) + x_msgs(z, 7, 2, 1):
        small.start()
    for j in (1, 2, 3):
        b2_send(0, j).start()
    lax.fori_loop(0, STEPS, start_own_v, 0)
    own_gate.start()

    own_seg.wait()
    for j in (1, 2, 3):
        seg_recv(j).wait_recv()

    def as_column(row):
        return jnp.transpose(jnp.broadcast_to(row, (HD, row.shape[1])))

    for s in range(NX):
        col_buf[pl.ds(lax.rem(s, 2) * TOK, TOK), :] = as_column(seg_buf[s].astype(F32))
        if s % 2 == 1:
            rows_ids = [seg_buf[s - 1].astype(F32), seg_buf[s].astype(F32)]

            def mask_rows(i, carry):
                rows = pl.ds(pl.multiple_of(i * 64, 64), 64)
                ids = col_buf[rows, :]
                for half in range(2):
                    for t in range(TOK // HD):
                        there = rows_ids[half][:, t * HD : (t + 1) * HD]
                        mask_buf[s // 2, rows, half * TOK + t * HD : half * TOK + (t + 1) * HD] = jnp.where(
                            ids == there, 1.0, 0.0
                        ).astype(BF16)
                return carry

            lax.fori_loop(0, BLK // 64, mask_rows, 0)

    def ways(k):
        return NZ - 1 if k % 2 else 1

    def serve_second(k):
        zh = head_z(k)
        for small in x_msgs(zh, k, k, 1):
            small.wait_recv()
        if k < 7:
            b_msg(zh, k, k, 1).wait_recv()
        else:
            b_half(zh, 0, 7, 7, 1).wait_recv()
            b_half(zh, HALF // 2, 7, 8, 1).wait_recv()
        if k <= 4:
            b_msg(zh, k, k + 2, ways(k)).start()
        elif k == 5:
            b_half(zh, 0, 5, 7, ways(k)).start()
        elif k == 6:
            b_half(zh, HALF // 2, 6, 8, ways(k)).start()
        if k <= 5:
            for small in x_msgs(zh, k, k + 2, ways(k)):
                small.start()
        for j in (1, 2, 3):
            b2_send(k, j).start()

    def serve_first(k, half):
        zh = head_z(k)
        a_msg(zh, half, 0, 2 * k + half, 1).wait_recv()
        if k <= 4 or k == 5 + half:
            to = 2 * (k + 2) + half if k <= 4 else 14 + half
            a_msg(zh, half, 2 * k + half, to, ways(k)).start()

    def across(k):
        for j in (1, 2, 3):
            b2_recv(k, j).wait_recv()
        c_send(k).start()

    for k in (1, 2):
        serve_second(k)
    own_a.wait()
    for j in (1, 2, 3):
        a1_recv(j).wait_recv()
    for half in (0, 1):
        a_msg(z, half, half, 2 + half, NZ - 1).start()
        a_msg(z, half, 14 + half, 4 + half, 1).start()
    for k in (3, 4, 5, 6):
        serve_second(k)
    across(0)
    serve_second(7)

    def compute(k):
        zh = head_z(k)
        for pair in (2, 3):

            @pl.when(k == 2 * pair - 2)
            def _():
                serve_first(2 * pair - 1, 0)
                serve_first(2 * pair, 0)

        own_v(k).wait()
        for j in (1, 2, 3):
            v_recv(k, j).wait_recv()
        gain = gain_buf[zh].astype(F32)
        bias = bias_buf[zh].astype(F32)
        for t in range(BLK // TOK):
            col_buf[pl.ds(t * TOK, TOK), :] = as_column(bias[:, t * TOK : (t + 1) * TOK])

        def norm_rows(i, carry):
            rows = pl.ds(pl.multiple_of(i * 128, 128), 128)
            act = gelu(v_buf[k, rows, :].astype(F32))
            scaled = act * lax.rsqrt(jnp.mean(act * act, axis=-1, keepdims=True) + EPSILON)
            vn_buf[rows, :] = (scaled * gain).astype(BF16)
            return carry

        lax.fori_loop(0, NX * TOK // 128, norm_rows, 0)

        @pl.when(k == 0)
        def _():
            serve_first(1, 0)
            serve_first(2, 0)

        c_recv(k).wait_recv()

        def mix_rows(i, carry):
            block, part = i // NY, lax.rem(i, NY)
            rows = pl.ds(pl.multiple_of(part * 256, 256), 256)
            matrix = m_buf[zh, part].reshape(256, BLK) * mask_buf[block, rows, :]
            values = vn_buf[pl.ds(pl.multiple_of(block * BLK, BLK), BLK), :]
            summed = jnp.dot(matrix, values, preferred_element_type=F32)
            r_buf[k, pl.ds(pl.multiple_of(block * BLK + part * 256, 256), 256), :] = (
                summed + col_buf[rows, :]
            ).astype(BF16)
            return carry

        lax.fori_loop(0, 2 * NY, mix_rows, 0)
        for j in (1, 3, 2):
            r_send(k, j).start()

    def step(k, carry):
        compute(k)
        for pair in (1, 2, 3):

            @pl.when(k == 2 * pair - 2)
            def _():
                serve_first(2 * pair - 1, 1)
                serve_first(2 * pair, 1)
                across(2 * pair - 1)
                across(2 * pair)

        @pl.when(k == 5)
        def _():
            serve_first(7, 0)
            serve_first(7, 1)
            across(7)

        return carry

    lax.fori_loop(0, STEPS, step, 0)

    def sent(k, carry):
        for j in (1, 2, 3):
            v_send(k, j).wait_send()
            b2_send(k, j).wait_send()
        c_send(k).wait_send()
        return carry

    lax.fori_loop(0, STEPS, sent, 0)
    for j in (1, 2, 3):
        seg_send(j).wait_send()
        a1_send(j).wait_send()
    for k in (0, 1, 2, 3, 4, 5, 6, 7, 8, 9, 10, 13, 14, 15):
        a_msg(z, 0, k, 0, 1).wait_send()
    for k in (0, 1, 2, 3, 4, 8):
        b_msg(z, k, 0, 1).wait_send()
    for k in (5, 6):
        b_half(z, 0, k, 0, 1).wait_send()
    for k in (0, 1, 2, 3, 4, 5, 7):
        for small in x_msgs(z, k, 0, 1):
            small.wait_send()

    own_gate.wait()

    def gate_rows(k, xs, source):
        cols = head_cols(k, xs)
        for i in range(TOK // 128):
            rows = pl.ds(i * 128, 128)
            gate = gelu(g_buf[rows, cols].astype(F32))
            out_ref[0, rows, cols] = (gate * source(i * 128).astype(F32)).astype(BF16)

    def own_gated(k, carry):
        gate_rows(
            k, x, lambda lo: r_buf[k, pl.ds(pl.multiple_of(x * TOK + lo, 128), 128), :]
        )
        return carry

    lax.fori_loop(0, STEPS, own_gated, 0)

    def gated(k, carry):
        for j in (1, 3, 2):
            r_recv(k, j).wait_recv()
            xs = lax.rem(x + NX - j, NX)
            gate_rows(k, xs, lambda lo: o_buf[xs, k, pl.ds(lo, 128), :])
        for j in (1, 3, 2):
            r_send(k, j).wait_send()
        return carry

    lax.fori_loop(0, STEPS, gated, 0)


def per_device(gate_in, value_in, segments, value_gain, mixing, mixing_bias):
    any_space = pl.BlockSpec(memory_space=pl.ANY)
    dma = pltpu.SemaphoreType.DMA
    return pl.pallas_call(
        kernel,
        out_shape=pltpu.VMEM(value_in.shape, BF16),
        in_specs=[any_space] * 6,
        out_specs=pl.BlockSpec(memory_space=pltpu.VMEM),
        scratch_shapes=[
            pltpu.VMEM((NZ, NY, NC, 2, HALF, BLK), BF16),
            pltpu.VMEM((STEPS, NX * TOK, HD), BF16),
            pltpu.VMEM((STEPS, NX * TOK, HD), BF16),
            pltpu.VMEM((NX, STEPS, TOK, HD), BF16),
            pltpu.VMEM((TOK, NX * NZ * HD), BF16),
            pltpu.VMEM((2, BLK, BLK), BF16),
            pltpu.VMEM((NX * TOK, HD), BF16),
            pltpu.VMEM((BLK, HD), F32),
            pltpu.VMEM((NX, 1, TOK), jnp.int32),
            pltpu.VMEM((NZ, 1, BLK), BF16),
            pltpu.VMEM((NZ, 1, HD), BF16),
            dma((6,)),
            dma((STEPS,)),
            dma((3,)),
            dma((3,)),
            dma((STEPS, 3)),
            dma((STEPS, 3)),
            dma((STEPS, 3)),
            dma((STEPS, 3)),
            dma((3,)),
            dma((3,)),
            dma((16,)),
            dma((16,)),
            dma((9,)),
            dma((9,)),
            dma((8,)),
            dma((8,)),
            dma((8,)),
            dma((8,)),
            dma((STEPS, 3)),
            dma((STEPS, 3)),
            dma((STEPS,)),
            dma((STEPS,)),
            pltpu.SemaphoreType.REGULAR,
            pltpu.SemaphoreType.REGULAR,
        ],
        compiler_params=pltpu.CompilerParams(
            collective_id=0, has_side_effects=True, vmem_limit_bytes=48 * 1024 * 1024
        ),
    )(*(pltpu.with_memory_space_constraint(a, pltpu.HBM) for a in (gate_in, value_in, segments, value_gain.reshape(1, HD), mixing, mixing_bias)))


def solution(mesh):
    return jax.shard_map(
        per_device,
        mesh=mesh,
        in_specs=(
            P("dp", "sp", None),
            P("dp", "sp", None),
            P("dp", "sp"),
            P("sp"),
            P("sp", "dp", None),
            P("sp", None),
        ),
        out_specs=P("dp", "sp", None),
        check_vma=False,
    )
```
